32 devices in a mesh: sp: 8 (over z, x), tp: 4 (over y, core).
Axes of the slice: x: 2, y: 2, z: 4, core: 2. Of those that a mesh axis runs over, the one named last changes fastest.
Arguments:
- queries: bfloat16 [1536, 1536], P('sp', 'tp'), may hold values from -64 to 64
- latents: bfloat16 [1536, 512], P('sp'), may hold values from -6 to 6
- rope_key: bfloat16 [1536, 32], P('sp'), may hold values from -64 to 64
- w_key: bfloat16 [512, 1024], P(None, 'tp'), may hold values from -0.25 to 0.25
- w_value: bfloat16 [512, 1024], P(None, 'tp'), may hold values from -0.25 to 0.25
- w_out: bfloat16 [1024, 2048], P('tp'), may hold values from -0.59765625 to 0.59765625
- resid: bfloat16 [1536, 2048], P('sp', 'tp'), may hold values from -12 to 12
- gain_mix: float32 [2048], P('tp'), may hold values from 0.1 to 1.9
- w_gate: bfloat16 [2048, 3072], P('sp', 'tp'), may hold values from -0.125 to 0.125
- w_up: bfloat16 [2048, 3072], P('sp', 'tp'), may hold values from -0.125 to 0.125
- w_down: bfloat16 [3072, 2048], P('tp', 'sp'), may hold values from -0.41992188 to 0.41992188
- gain_out: float32 [2048], P('tp'), may hold values from 0.1 to 1.9
Outputs:
- layer_out: bfloat16 [1536, 2048], P('sp', 'tp')
The draws below stay inside these ranges and needn't reach their ends.
All inputs are finite; a program needn't handle non-finite values.
Results may differ from the reference program's by a relative error of at most 0.014.
Values may be sent and summed in bfloat16 or wider, within the bound.
A program may use at most 128 MiB of HBM per device.

```python
import math
import jax
import jax.numpy as jnp
from jax import lax

D = 2048
HEADS = 16
NOPE = 64
ROPE = 32
VDIM = 64
KV_RANK = 512
FF = 3072
GRID_W = 64
TOKENS = 1536
N_TP = 4


def drawn_pair(key):
    query_seed = jax.random.fold_in(key, 11)
    rotary_seed = jax.random.fold_in(key, 12)
    width_total = HEADS * (NOPE + ROPE)
    queries = jnp.clip(jax.random.normal(query_seed, (TOKENS, width_total), jnp.float32) * 2.5, -15.0, 15.0)
    rotary = jnp.clip(jax.random.normal(rotary_seed, (TOKENS, ROPE), jnp.float32), -6.0, 6.0)
    return (queries, rotary)


def draw_queries(key, part):
    return drawn_pair(key)[0].astype(jnp.bfloat16)


def draw_rope_key(key, part):
    return drawn_pair(key)[1].astype(jnp.bfloat16)


def draw_resid(key, part):
    row_seed = jax.random.fold_in(key, 21)
    value_seed = jax.random.fold_in(key, 22)
    column_scale = 0.6 * 10.0 ** (jnp.arange(D, dtype=jnp.float32) / (D - 1) - 0.5)
    row_scale = 10.0 ** jax.random.uniform(row_seed, (TOKENS, 1), jnp.float32, -0.5, 0.5)
    values_out = jax.random.normal(value_seed, (TOKENS, D), jnp.float32) * row_scale * column_scale
    return jnp.clip(values_out, -12.0, 12.0).astype(jnp.bfloat16)


def steps_of(key, shape, cuts, low, largest):
    gain, own = 1.0, jax.random.fold_in(key, 6)
    for axis_at, shards_of in cuts:
        draws = jnp.exp(jax.random.uniform(jax.random.fold_in(own, axis_at), (shards_of,), jnp.float32, low / len(cuts), largest / len(cuts)))
        gain = gain * jnp.repeat(draws, shape[axis_at] // shards_of).reshape([-1 if axis == axis_at else 1 for axis in range(len(shape))])
    return gain


def gaussian(stream_key, shape, spread, limit, pieces=(), kind=jnp.bfloat16):
    result = jax.random.normal(stream_key, shape, jnp.float32) * spread
    if len(pieces) > 0:
        result = steps_of(stream_key, shape, pieces, -0.22, 0.18) * result
    return jnp.clip(result, min=-limit, max=limit).astype(kind)


def setup_inputs(seed: int = 0) -> dict:
    keys = jax.random.split(jax.random.key(seed), 13)
    queries = draw_queries(jax.random.fold_in(keys[12], 71), 0)
    latents = gaussian(keys[1], (TOKENS, KV_RANK), 1.0, 6.0, ((0, 8),))
    rope_key = draw_rope_key(jax.random.fold_in(keys[12], 71), 0)
    w_key = gaussian(keys[3], (KV_RANK, HEADS * NOPE), KV_RANK ** -0.5, 0.25, ((1, 4),))
    w_value = gaussian(keys[4], (KV_RANK, HEADS * VDIM), KV_RANK ** -0.5, 0.25, ((1, 4),))
    w_out = gaussian(keys[5], (HEADS * VDIM, D), 0.1, 0.59765625, ((0, 4),))
    resid = draw_resid(jax.random.fold_in(keys[12], 71), 0)
    gain_mix = jnp.clip(1.0 + 0.18 * jax.random.normal(keys[7], (D,), jnp.float32), 0.1, 1.9)
    w_gate = gaussian(keys[8], (D, FF), D ** -0.5, 0.125, ((0, 8), (1, 4)))
    w_up = gaussian(keys[9], (D, FF), D ** -0.5, 0.125, ((0, 8), (1, 4)))
    w_down = gaussian(keys[10], (FF, D), 0.07, 0.41992188, ((0, 4), (1, 8)))
    gain_out = jnp.clip(1.0 + 0.18 * jax.random.normal(keys[11], (D,), jnp.float32), 0.1, 1.9)
    return {"queries": queries, "latents": latents, "rope_key": rope_key, "w_key": w_key, "w_value": w_value, "w_out": w_out, "resid": resid, "gain_mix": gain_mix, "w_gate": w_gate, "w_up": w_up, "w_down": w_down, "gain_out": gain_out}


ROTARY_BASE = 10000.0
NORM_EPSILON = 1e-06
DEEP_ALPHA = 8.0 ** 0.25
HALF_STEP = 0.5

def rotary_tables(positions, rotary_width, grid_width):
    grid_rows = (positions // grid_width).astype(jnp.float32)
    grid_cols = (positions % grid_width).astype(jnp.float32)
    freq_count = rotary_width // 4
    inverse = ROTARY_BASE ** (-jnp.arange(freq_count, dtype=jnp.float32) / freq_count)
    angle_table = jnp.concatenate([grid_rows[:, None] * inverse, grid_cols[:, None] * inverse], axis=-1)
    return (jnp.cos(angle_table), jnp.sin(angle_table))

def rotate(vectors, cosine, sine):
    half_width = vectors.shape[-1] // 2
    leading = vectors[..., :half_width].astype(jnp.float32)
    trailing = vectors[..., half_width:].astype(jnp.float32)
    return jnp.concatenate([leading * cosine - trailing * sine, leading * sine + trailing * cosine], axis=-1).astype(jnp.bfloat16)

def widened(tensor):
    return lax.optimization_barrier(tensor.astype(jnp.bfloat16)).astype(jnp.float32)

def layer_norm(rows_in, gain_row):
    row_mean = lax.optimization_barrier(jnp.mean(rows_in, axis=1, keepdims=True))
    variance = lax.optimization_barrier(jnp.mean(rows_in * rows_in, axis=1, keepdims=True)) - row_mean * row_mean
    return ((rows_in - row_mean) * lax.rsqrt(variance + NORM_EPSILON) * gain_row.astype(jnp.float32)).astype(jnp.bfloat16)

def group_sum(left, right, group_width):
    total_sum = jnp.zeros((left.shape[0], right.shape[1]), jnp.float32)
    for group_index in range(N_TP):
        lower = group_index * group_width
        partial_term = jnp.dot(left[:, lower:lower + group_width], right[lower:lower + group_width], preferred_element_type=jnp.float32)
        total_sum = total_sum + widened(partial_term)
    return total_sum

def reference(queries, latents, rope_key, w_key, w_value, w_out, resid, gain_mix, w_gate, w_up, w_down, gain_out):
    positions = jnp.arange(TOKENS, dtype=jnp.int32)
    cosine, sine = rotary_tables(positions, ROPE, GRID_W)
    key_rot = lax.optimization_barrier(rotate(rope_key, cosine, sine)).astype(jnp.float32)
    shaped = queries.reshape(TOKENS, HEADS, NOPE + ROPE)
    q_nope = shaped[:, :, :NOPE]
    q_rot = rotate(shaped[:, :, NOPE:], cosine[:, None, :], sine[:, None, :])
    key_nope = widened(jnp.dot(latents, w_key, preferred_element_type=jnp.float32)).reshape(TOKENS, HEADS, NOPE)
    head_values = widened(jnp.dot(latents, w_value, preferred_element_type=jnp.float32)).reshape(TOKENS, HEADS, VDIM)
    block_rows = math.gcd(TOKENS, 512)
    score_scale = (NOPE + ROPE) ** (-0.5)

    def attend(block_index):
        first_row = (block_index * block_rows).astype(jnp.int32)
        query_nope = lax.dynamic_slice_in_dim(q_nope, first_row, block_rows, 0).astype(jnp.float32)
        query_rope = lax.dynamic_slice_in_dim(q_rot, first_row, block_rows, 0).astype(jnp.float32)
        scores = jnp.einsum('qhd,khd->hqk', query_nope, key_nope) + jnp.einsum('qhd,kd->hqk', query_rope, key_rot)
        scores = scores * score_scale
        row_max = lax.optimization_barrier(jnp.max(scores, axis=-1, keepdims=True))
        weights = jnp.exp(scores - row_max)
        totals = lax.optimization_barrier(jnp.sum(weights, axis=-1))
        prob_weights = widened(weights)
        heads_block = jnp.einsum('hqk,khd->qhd', prob_weights, head_values) / jnp.transpose(totals)[:, :, None]
        return heads_block.astype(jnp.bfloat16).reshape(block_rows, HEADS * VDIM)
    heads_out = lax.map(attend, jnp.arange(TOKENS // block_rows, dtype=jnp.int32)).reshape(TOKENS, HEADS * VDIM)
    attn_sum = group_sum(heads_out, w_out, HEADS * VDIM // N_TP)
    mixed_in = DEEP_ALPHA * resid.astype(jnp.float32) + attn_sum
    hidden_in = layer_norm(mixed_in, gain_mix)
    gate_sum = jnp.dot(hidden_in, w_gate, preferred_element_type=jnp.float32)
    up_sum = jnp.dot(hidden_in, w_up, preferred_element_type=jnp.float32)
    hidden = (jax.nn.silu(gate_sum) * up_sum).astype(jnp.bfloat16)
    mixer_sum = group_sum(hidden, w_down, FF // N_TP)
    return layer_norm(DEEP_ALPHA * hidden_in.astype(jnp.float32) + HALF_STEP * mixer_sum, gain_out)
```

```python
import functools

import jax
import jax.numpy as jnp
from jax import lax
from jax.experimental import pallas as pl
from jax.experimental.pallas import tpu as pltpu
from jax.sharding import PartitionSpec as P

NOPE = 64
ROPE = 32
VDIM = 64
GRID_W = 64
LANES = 128

ROTARY_BASE = 10000.0
NORM_EPSILON = 1e-06
DEEP_ALPHA = 8.0**0.25
HALF_STEP = 0.5
MESH = pl.DeviceIdType.MESH


def rotary_tables(positions, rotary_width, grid_width):
    grid_rows = (positions // grid_width).astype(jnp.float32)
    grid_cols = (positions % grid_width).astype(jnp.float32)
    freq_count = rotary_width // 4
    inverse = ROTARY_BASE ** (-jnp.arange(freq_count, dtype=jnp.float32) / freq_count)
    angle_table = jnp.concatenate(
        [grid_rows[:, None] * inverse, grid_cols[:, None] * inverse], axis=-1
    )
    return (jnp.cos(angle_table), jnp.sin(angle_table))


def rotate(vectors, cosine, sine):
    half_width = vectors.shape[-1] // 2
    leading = vectors[..., :half_width].astype(jnp.float32)
    trailing = vectors[..., half_width:].astype(jnp.float32)
    return jnp.concatenate(
        [leading * cosine - trailing * sine, leading * sine + trailing * cosine], axis=-1
    ).astype(jnp.bfloat16)


def ring_device(place, count):
    return jnp.where(place < count // 2, 2 * place, 2 * (count - 1 - place) + 1)


def ring_place(index, count):
    return jnp.where(index % 2 == 0, index // 2, count - 1 - index // 2)


def dot(left, right):
    return jnp.dot(left, right, preferred_element_type=jnp.float32)


def dot_nt(left, right):
    return lax.dot_general(
        left, right, (((1,), (1,)), ((), ())), preferred_element_type=jnp.float32
    )


def layer_kernel(
    n_sp,
    n_tp,
    splits,
    q_ref,
    lat_ref,
    wk_ref,
    wv_ref,
    wo_ref,
    resid_ref,
    gain_mix_ref,
    gain_out_ref,
    wg_ref,
    wu_ref,
    wd_ref,
    out_ref,
    lat_all,
    keys,
    values,
    gate_all,
    up_all,
    down_all,
    heads,
    part_send,
    part_recv,
    stat_send,
    stat_recv,
    rows_all,
    part2_send,
    part2_recv,
    stat2_send,
    stat2_recv,
    local_sem,
    lat_send,
    lat_recv,
    share_send,
    share_recv,
    ring_send,
    ring_recv,
    tp_send,
    tp_recv,
):
    sp = lax.axis_index("sp")
    tp = lax.axis_index("tp")
    place = ring_place(sp, n_sp)
    ahead = ring_device((place + 1) % n_sp, n_sp)
    behind = ring_device((place + n_sp - 1) % n_sp, n_sp)
    targets = (ahead, behind)
    partner = tp + 1 - 2 * (tp % 2)
    core = tp % 2
    n_rows = q_ref.shape[1]
    head_count = q_ref.shape[0]
    lat_rows = lat_all.shape[2]
    n_cols = out_ref.shape[1]

    own = []
    lat_own = pltpu.make_async_copy(lat_ref, lat_all.at[sp], local_sem.at[0])
    lat_own.start()
    weights = (gate_all, up_all, down_all)
    for i, (source, target) in enumerate(
        zip((wg_ref, wu_ref, wd_ref), weights)
    ):
        copy = pltpu.make_async_copy(source, target.at[sp], local_sem.at[i + 1])
        copy.start()
        own.append(copy)

    barrier = pltpu.get_barrier_semaphore()
    for device in targets:
        pl.semaphore_signal(barrier, inc=1, device_id={"sp": device}, device_id_type=MESH)
    for step in range(1, n_tp):
        pl.semaphore_signal(
            barrier, inc=1, device_id={"tp": (tp + step) % n_tp}, device_id_type=MESH
        )
    pl.semaphore_wait(barrier, 2 + n_tp - 1)

    def origin(hop, direction):
        if direction == 0:
            return ring_device((place + n_sp - hop) % n_sp, n_sp)
        return ring_device((place + hop) % n_sp, n_sp)

    def lat_copy(hop, direction):
        block = lat_all.at[origin(hop - 1, direction), core * 2 + direction]
        return pltpu.make_async_remote_copy(
            src_ref=block,
            dst_ref=block,
            send_sem=lat_send.at[direction],
            recv_sem=lat_recv.at[direction, hop - 1],
            device_id={"sp": targets[direction]},
            device_id_type=MESH,
        )

    def lat_arrival(hop, direction):
        block = lat_all.at[origin(hop, direction), core * 2 + direction]
        return pltpu.make_async_remote_copy(
            src_ref=block,
            dst_ref=block,
            send_sem=lat_send.at[direction],
            recv_sem=lat_recv.at[direction, hop - 1],
            device_id={"sp": targets[direction]},
            device_id_type=MESH,
        )

    def share_copy(hop, direction, which):
        block = lat_all.at[origin(hop, direction), which * 2 + direction]
        return pltpu.make_async_remote_copy(
            src_ref=block,
            dst_ref=block,
            send_sem=share_send.at[direction],
            recv_sem=share_recv.at[direction, hop - 1],
            device_id={"tp": partner},
            device_id_type=MESH,
        )

    piece_rows = wg_ref.shape[0] // (2 * splits)

    def ring_copy(array, piece, hop, direction, arriving):
        block = origin(hop if arriving else hop - 1, direction)
        rows = pl.ds((direction * splits + piece) * piece_rows, piece_rows)
        ref = weights[array].at[block, rows]
        return pltpu.make_async_remote_copy(
            src_ref=ref,
            dst_ref=ref,
            send_sem=ring_send.at[array, piece, direction],
            recv_sem=ring_recv.at[array, piece, direction, hop - 1],
            device_id={"sp": targets[direction]},
            device_id_type=MESH,
        )

    started = set()

    def ring_step(array, piece, hop):
        if hop == 1 and array not in started:
            own[array].wait()
            started.add(array)
        for direction in range(2):
            if hop > 1:
                ring_copy(array, piece, hop - 1, direction, True).wait_recv()
                ring_copy(array, piece, hop - 1, direction, False).wait_send()
            if hop < n_sp:
                ring_copy(array, piece, hop, direction, False).start()

    first = [
        (array, piece, hop)
        for hop in range(1, n_sp)
        for array in range(2)
        for piece in range(splits)
    ]
    second = [(2, piece, hop) for hop in range(1, n_sp) for piece in range(splits)]
    queue = [first + second, 0]

    def advance(count):
        steps, at = queue
        for step in steps[at : at + count]:
            ring_step(*step)
        queue[1] = min(at + count, len(steps))

    unit = max(1, len(first) // 28)

    lat_own.wait()
    for hop in range(1, n_sp + 1):
        for direction in range(2):
            if hop > 1:
                lat_arrival(hop - 1, direction).wait_recv()
                lat_copy(hop - 1, direction).wait_send()
            if hop < n_sp:
                lat_copy(hop, direction).start()
            if hop > 2:
                share_copy(hop - 2, direction, core).wait_send()
            if hop > 1:
                share_copy(hop - 1, direction, core).start()
        if hop < n_sp and queue[1] < 7 * unit:
            advance(1)
    for direction in range(2):
        share_copy(n_sp - 1, direction, core).wait_send()
        for hop in range(1, n_sp):
            share_copy(hop, direction, 1 - core).wait_recv()

    total_rows = n_sp * n_rows
    lat_wide = lat_all.shape[3]
    chunk_blocks = max(1, min(n_sp, 1536 // n_rows))
    chunks = n_sp // chunk_blocks
    chunk = chunk_blocks * n_rows
    half_blocks = max(1, chunk_blocks // 2)

    def project(step):
        rows = half_blocks * n_rows
        lat = lat_all[pl.ds(step * half_blocks, half_blocks)].reshape(rows, lat_wide)
        keys[pl.ds(step * rows, rows)] = dot(lat, wk_ref[...]).astype(jnp.bfloat16)
        values[pl.ds(step * rows, rows)] = dot(lat, wv_ref[...]).astype(jnp.bfloat16)

    if chunks == 1:
        for step in range(n_sp // half_blocks):
            project(step)
            advance(unit)
    else:
        pl.loop(0, n_sp // half_blocks)(project)
        advance(2 * unit)

    score_scale = (NOPE + ROPE) ** (-0.5)
    lane = lax.broadcasted_iota(jnp.int32, (n_rows, LANES), 1)

    def attend(head, at, state):
        maxima, totals, running = state
        rows = pl.ds(at * chunk, chunk)
        columns = slice(head * LANES, (head + 1) * LANES)
        pair = slice(head // 2 * LANES, (head // 2 + 1) * LANES)
        scores = dot_nt(q_ref[head], keys[rows, columns]) * score_scale
        top = jnp.max(scores, axis=1, keepdims=True)
        if maxima is not None:
            top = jnp.maximum(maxima, top)
        probs = jnp.exp(scores - top)
        sums = jnp.sum(probs, axis=1, keepdims=True)
        update = dot(probs.astype(jnp.bfloat16), values[rows, pair])
        if maxima is not None:
            factor = jnp.exp(maxima - top)
            sums = totals * factor + sums
            update = running * factor + update
        return (top, sums, update)

    for head in range(head_count):
        state = attend(head, 0, (None, None, None))
        if chunks > 1:
            state = lax.fori_loop(1, chunks, functools.partial(attend_loop, attend, head), state)
        result = state[2] / state[1]
        pair = slice(head // 2 * LANES, (head // 2 + 1) * LANES)
        if head % 2 == 0:
            heads[:, pair] = result.astype(jnp.bfloat16)
        else:
            heads[:, pair] = jnp.where(
                lane < VDIM, heads[:, pair].astype(jnp.float32), result
            ).astype(jnp.bfloat16)
        advance(unit)

    def tp_copy(stage, slot_source, slot_target, to, slot_semaphore):
        return pltpu.make_async_remote_copy(
            src_ref=slot_source,
            dst_ref=slot_target,
            send_sem=tp_send.at[stage, slot_semaphore],
            recv_sem=tp_recv.at[stage, slot_semaphore],
            device_id={"tp": to},
            device_id_type=MESH,
        )

    def exchange(stage, source_of, target_of):
        copies = []
        for k in range(1, n_tp):
            to = (tp + k) % n_tp
            copies.append(tp_copy(stage, source_of(to), target_of(k), to, k))
        return copies

    copies = exchange(0, lambda to: part_send.at[to], lambda k: part_recv.at[k])
    for k in range(1, n_tp + 1):
        to = (tp + k) % n_tp
        part_send[to] = dot(
            heads[...], wo_ref[:, pl.ds(pl.multiple_of(to * n_cols, LANES), n_cols)]
        ).astype(jnp.bfloat16)
        if k < n_tp:
            copies[k - 1].start()
    advance(4 * unit)
    mixed = DEEP_ALPHA * resid_ref[...].astype(jnp.float32) + part_send[tp].astype(jnp.float32)
    for k in range(1, n_tp):
        copies[k - 1].wait_recv()
        mixed = mixed + part_recv[k].astype(jnp.float32)
    pending = list(copies)

    width_total = n_cols * n_tp

    def normed(rows_in, gain_ref, stage, send, recv, between):
        sums = jnp.sum(rows_in, axis=1, keepdims=True)
        squares = jnp.sum(rows_in * rows_in, axis=1, keepdims=True)
        mine = jnp.where(lane < LANES // 2, sums, squares)
        send[...] = mine
        copies = exchange(stage, lambda to: send, lambda k: recv.at[k])
        for copy in copies:
            copy.start()
        between()
        for k in range(1, n_tp):
            copies[k - 1].wait_recv()
            mine = mine + recv[k]
        pending.extend(copies)
        row_mean = mine[:, :1] / width_total
        variance = mine[:, LANES // 2 : LANES // 2 + 1] / width_total - row_mean * row_mean
        return (
            (rows_in - row_mean) * lax.rsqrt(variance + NORM_EPSILON) * gain_ref[...]
        ).astype(jnp.bfloat16)

    hidden_in = normed(
        mixed, gain_mix_ref, 1, stat_send, stat_recv, lambda: advance(2 * unit)
    )
    rows_all[tp] = hidden_in
    copies = exchange(2, lambda to: rows_all.at[tp], lambda k: rows_all.at[tp])
    for copy in copies:
        copy.start()
    pending.extend(copies)
    advance(4 * unit)
    for k in range(1, n_tp):
        sender = (tp + n_tp - k) % n_tp
        tp_copy(2, rows_all.at[sender], rows_all.at[sender], sender, k).wait_recv()

    advance(len(first) - queue[1])
    advance(splits)

    def last_hop(array):
        for piece in range(splits):
            for direction in range(2):
                ring_copy(array, piece, n_sp - 1, direction, True).wait_recv()
                ring_copy(array, piece, n_sp - 1, direction, False).wait_send()

    last_hop(0)
    group = n_sp // n_tp
    depth = group * wg_ref.shape[0]
    hidden_width = wg_ref.shape[1]

    def wide(weight):
        total = None
        for t in range(n_tp):
            term = dot(
                rows_all[t],
                weight[t * group : (t + 1) * group].reshape(depth, hidden_width),
            )
            total = term if total is None else total + term
        return total

    gate_sum = wide(gate_all)
    advance(splits)
    last_hop(1)
    up_sum = wide(up_all)
    advance(splits)
    hidden = (gate_sum / (1.0 + jnp.exp(-gate_sum)) * up_sum).astype(jnp.bfloat16)

    advance(len(queue[0]))
    last_hop(2)
    copies = exchange(3, lambda to: part2_send.at[to], lambda k: part2_recv.at[k])
    for k in range(1, n_tp + 1):
        to = (tp + k) % n_tp
        part2_send[to] = dot_nt(
            hidden, down_all[pl.ds(to * group, group)].reshape(depth, hidden_width)
        ).astype(jnp.bfloat16)
        if k < n_tp:
            copies[k - 1].start()
    mixer = part2_send[tp].astype(jnp.float32)
    for k in range(1, n_tp):
        copies[k - 1].wait_recv()
        mixer = mixer + part2_recv[k].astype(jnp.float32)
    pending.extend(copies)
    final = DEEP_ALPHA * rows_all[tp].astype(jnp.float32) + HALF_STEP * mixer
    out_ref[...] = normed(final, gain_out_ref, 4, stat2_send, stat2_recv, lambda: None)
    for copy in pending:
        copy.wait_send()


def attend_loop(attend, head, at, state):
    return attend(head, at, state)


def local(
    queries,
    latents,
    rope_key,
    w_key,
    w_value,
    w_out,
    resid,
    gain_mix,
    w_gate,
    w_up,
    w_down,
    gain_out,
):
    n_sp = lax.axis_size("sp")
    n_tp = lax.axis_size("tp")
    rows = queries.shape[0]
    head_count = w_key.shape[1] // NOPE
    rank = latents.shape[1]
    cols = resid.shape[1]
    hidden_width = w_gate.shape[1]
    weight_rows = w_gate.shape[0]
    offset = lax.axis_index("sp") * rows
    positions = offset + jnp.arange(rows, dtype=jnp.int32)
    cosine, sine = rotary_tables(positions, ROPE, GRID_W)
    key_rot = rotate(rope_key, cosine, sine)
    shaped = queries.reshape(rows, head_count, NOPE + ROPE)
    q_rot = rotate(shaped[:, :, NOPE:], cosine[:, None, :], sine[:, None, :])
    spare = LANES - NOPE - ROPE
    q_pad = jnp.concatenate(
        [shaped[:, :, :NOPE], q_rot, jnp.zeros((rows, head_count, spare), jnp.bfloat16)], axis=-1
    )
    q_pad = jnp.transpose(q_pad, (1, 0, 2))
    lat_wide = rank + LANES
    lat_ext = jnp.concatenate(
        [latents, key_rot, jnp.zeros((rows, LANES - ROPE), jnp.bfloat16)], axis=1
    ).reshape(4, rows // 4, lat_wide)
    key_cols = jnp.pad(
        w_key.reshape(rank, head_count, NOPE), ((0, LANES), (0, 0), (0, LANES - NOPE))
    )
    place_rot = jnp.pad(
        jnp.eye(ROPE, dtype=jnp.bfloat16), ((rank, LANES - ROPE), (NOPE, spare))
    )
    key_cols = (key_cols + place_rot[:, None, :]).reshape(lat_wide, head_count * LANES)
    value_cols = jnp.pad(w_value, ((0, LANES), (0, 0)))
    splits = 2 if weight_rows % 64 == 0 else 1
    bf16 = jnp.bfloat16
    total_rows = n_sp * rows
    vmem = pl.BlockSpec(memory_space=pltpu.VMEM)
    anywhere = pl.BlockSpec(memory_space=pl.ANY)
    dma = pltpu.SemaphoreType.DMA
    return pl.pallas_call(
        functools.partial(layer_kernel, n_sp, n_tp, splits),
        out_shape=jax.ShapeDtypeStruct((rows, cols), bf16),
        in_specs=[vmem, anywhere] + [vmem] * 6 + [anywhere] * 3,
        out_specs=vmem,
        scratch_shapes=[
            pltpu.VMEM((n_sp, 4, rows // 4, lat_wide), bf16),
            pltpu.VMEM((total_rows, head_count * LANES), bf16),
            pltpu.VMEM((total_rows, head_count * VDIM), bf16),
            pltpu.VMEM((n_sp, weight_rows, hidden_width), bf16),
            pltpu.VMEM((n_sp, weight_rows, hidden_width), bf16),
            pltpu.VMEM((n_sp, weight_rows, hidden_width), bf16),
            pltpu.VMEM((rows, head_count * VDIM), bf16),
            pltpu.VMEM((n_tp, rows, cols), bf16),
            pltpu.VMEM((n_tp, rows, cols), bf16),
            pltpu.VMEM((rows, LANES), jnp.float32),
            pltpu.VMEM((n_tp, rows, LANES), jnp.float32),
            pltpu.VMEM((n_tp, rows, cols), bf16),
            pltpu.VMEM((n_tp, rows, cols), bf16),
            pltpu.VMEM((n_tp, rows, cols), bf16),
            pltpu.VMEM((rows, LANES), jnp.float32),
            pltpu.VMEM((n_tp, rows, LANES), jnp.float32),
            dma((4,)),
            dma((2,)),
            dma((2, n_sp - 1)),
            dma((2,)),
            dma((2, n_sp - 1)),
            dma((3, splits, 2)),
            dma((3, splits, 2, n_sp - 1)),
            dma((5, n_tp)),
            dma((5, n_tp)),
        ],
        compiler_params=pltpu.CompilerParams(
            collective_id=0, has_side_effects=True, vmem_limit_bytes=66000000
        ),
    )(
        q_pad,
        lat_ext,
        key_cols,
        value_cols,
        w_out,
        resid,
        gain_mix.reshape(1, -1),
        gain_out.reshape(1, -1),
        w_gate,
        w_up,
        w_down.T,
    )


def solution(mesh):
    placed = (
        P("sp", "tp"),
        P("sp", None),
        P("sp", None),
        P(None, "tp"),
        P(None, "tp"),
        P("tp", None),
        P("sp", "tp"),
        P("tp"),
        P("sp", "tp"),
        P("sp", "tp"),
        P("tp", "sp"),
        P("tp"),
    )
    return jax.shard_map(
        local, mesh=mesh, in_specs=placed, out_specs=P("sp", "tp"), check_vma=False
    )
```

```python
import functools

import jax
import jax.numpy as jnp
from jax import lax
from jax.experimental import pallas as pl
from jax.experimental.pallas import tpu as pltpu
from jax.sharding import PartitionSpec as P

NOPE = 64
ROPE = 32
VDIM = 64
GRID_W = 64
LANES = 128

ROTARY_BASE = 10000.0
NORM_EPSILON = 1e-06
DEEP_ALPHA = 8.0**0.25
HALF_STEP = 0.5
MESH = pl.DeviceIdType.MESH


def rotary_tables(first, rows):
    at = first + lax.broadcasted_iota(jnp.int32, (rows, LANES), 0)
    column = lax.broadcasted_iota(jnp.int32, (rows, LANES), 1)
    freq_count = ROPE // 4
    grid_row = (at // GRID_W).astype(jnp.float32)
    grid_col = (at % GRID_W).astype(jnp.float32)
    spot = jnp.where(column % (2 * freq_count) < freq_count, grid_row, grid_col)
    inverse = jnp.ones((rows, LANES), jnp.float32)
    for k in range(1, freq_count):
        inverse = jnp.where(column % freq_count == k, ROTARY_BASE ** (-k / freq_count), inverse)
    angles = spot * inverse
    return (jnp.cos(angles)[:, : ROPE // 2], jnp.sin(angles)[:, : ROPE // 2])


def rotate(vectors, cosine, sine):
    half_width = ROPE // 2
    leading = vectors[:, :half_width]
    trailing = vectors[:, half_width:]
    return [leading * cosine - trailing * sine, leading * sine + trailing * cosine]


def ring_device(place, count):
    return jnp.where(place < count // 2, 2 * place, 2 * (count - 1 - place) + 1)


def ring_place(index, count):
    return jnp.where(index % 2 == 0, index // 2, count - 1 - index // 2)


def dot(left, right):
    return jnp.dot(left, right, preferred_element_type=jnp.float32)


def dot_nt(left, right):
    return lax.dot_general(
        left, right, (((1,), (1,)), ((), ())), preferred_element_type=jnp.float32
    )


def layer_kernel(
    n_sp,
    n_tp,
    splits,
    q_ref,
    lat_ref,
    rope_ref,
    wk_ref,
    wv_ref,
    wo_ref,
    resid_ref,
    gain_mix_ref,
    gain_out_ref,
    wg_ref,
    wu_ref,
    wd_ref,
    out_ref,
    lat_all,
    keys,
    rotary,
    values,
    gate_all,
    up_all,
    down_all,
    q_all,
    heads,
    part_send,
    part_recv,
    stat_send,
    stat_recv,
    rows_all,
    part2_send,
    part2_recv,
    stat2_send,
    stat2_recv,
    hid,
    local_sem,
    lat_send,
    lat_recv,
    share_send,
    share_recv,
    ring_send,
    ring_recv,
    tp_send,
    tp_recv,
    down_send,
    down_recv,
):
    sp = lax.axis_index("sp")
    tp = lax.axis_index("tp")
    place = ring_place(sp, n_sp)
    ahead = ring_device((place + 1) % n_sp, n_sp)
    behind = ring_device((place + n_sp - 1) % n_sp, n_sp)
    targets = (ahead, behind)
    partner = tp + 1 - 2 * (tp % 2)
    core = tp % 2
    n_rows = q_ref.shape[0]
    head_count = wk_ref.shape[1] // NOPE
    rank = wk_ref.shape[0]
    lat_rows = lat_all.shape[2]
    n_cols = out_ref.shape[1]

    barrier = pltpu.get_barrier_semaphore()
    for device in targets:
        pl.semaphore_signal(barrier, inc=1, device_id={"sp": device}, device_id_type=MESH)
    for step in range(1, n_tp):
        pl.semaphore_signal(
            barrier, inc=1, device_id={"tp": (tp + step) % n_tp}, device_id_type=MESH
        )

    own = []
    lat_own = pltpu.make_async_copy(
        lat_ref, lat_all.at[sp, :, :, pl.ds(0, rank)], local_sem.at[0]
    )
    lat_own.start()
    weights = (gate_all, up_all, down_all)
    for i, source in enumerate((wg_ref, wu_ref)):
        copy = pltpu.make_async_copy(source, weights[i].at[sp], local_sem.at[i + 1])
        copy.start()
        own.append(copy)
    cosine, sine = rotary_tables(sp * n_rows, n_rows)
    key_rot = rotate(rope_ref[...].astype(jnp.float32), cosine, sine)
    key_rot.append(jnp.zeros((n_rows, LANES - ROPE), jnp.float32))
    lat_all[sp, :, :, pl.ds(rank, LANES)] = (
        jnp.concatenate(key_rot, axis=1).astype(jnp.bfloat16).reshape(4, lat_rows, LANES)
    )

    def prepare_queries(head):
        base = head * (NOPE + ROPE)
        wide_q = q_ref[...].astype(jnp.float32)
        nope = wide_q[:, base : base + NOPE]
        other = jnp.zeros((n_rows, NOPE), jnp.float32)
        rotary = rotate(wide_q[:, base + NOPE : base + NOPE + ROPE], cosine, sine)
        parts = [nope, other] if head % 2 == 0 else [other, nope]
        parts = parts + rotary + [jnp.zeros((n_rows, LANES - ROPE), jnp.float32)]
        q_all[head] = jnp.concatenate(parts, axis=1).astype(jnp.bfloat16)

    def prepare_down():
        count = wd_ref.shape[1]
        across = lax.broadcasted_iota(jnp.int32, (count, count), 1)
        diagonal = (lax.broadcasted_iota(jnp.int32, (count, count), 0) == across).astype(
            jnp.float32
        ).astype(jnp.bfloat16)
        down_all[sp] = dot_nt(diagonal, wd_ref[...]).astype(jnp.bfloat16)

    preparing = [functools.partial(prepare_queries, head) for head in range(head_count)]
    preparing.append(prepare_down)
    pl.semaphore_wait(barrier, 2 + n_tp - 1)

    def origin(hop, direction):
        if direction == 0:
            return ring_device((place + n_sp - hop) % n_sp, n_sp)
        return ring_device((place + hop) % n_sp, n_sp)

    def lat_copy(hop, direction):
        block = lat_all.at[origin(hop - 1, direction), core * 2 + direction]
        return pltpu.make_async_remote_copy(
            src_ref=block,
            dst_ref=block,
            send_sem=lat_send.at[direction],
            recv_sem=lat_recv.at[direction, hop - 1],
            device_id={"sp": targets[direction]},
            device_id_type=MESH,
        )

    def lat_arrival(hop, direction):
        block = lat_all.at[origin(hop, direction), core * 2 + direction]
        return pltpu.make_async_remote_copy(
            src_ref=block,
            dst_ref=block,
            send_sem=lat_send.at[direction],
            recv_sem=lat_recv.at[direction, hop - 1],
            device_id={"sp": targets[direction]},
            device_id_type=MESH,
        )

    def share_copy(hop, direction, which):
        block = lat_all.at[origin(hop, direction), which * 2 + direction]
        return pltpu.make_async_remote_copy(
            src_ref=block,
            dst_ref=block,
            send_sem=share_send.at[direction],
            recv_sem=share_recv.at[direction, hop - 1],
            device_id={"tp": partner},
            device_id_type=MESH,
        )

    piece_rows = wg_ref.shape[0] // (2 * splits)

    def ring_copy(array, piece, hop, direction, arriving):
        block = origin(hop if arriving else hop - 1, direction)
        rows = pl.ds((direction * splits + piece) * piece_rows, piece_rows)
        ref = weights[array].at[block, rows]
        return pltpu.make_async_remote_copy(
            src_ref=ref,
            dst_ref=ref,
            send_sem=ring_send.at[array, piece, direction],
            recv_sem=ring_recv.at[array, piece, direction, hop - 1],
            device_id={"sp": targets[direction]},
            device_id_type=MESH,
        )

    started = set()

    def ring_step(array, piece, hop):
        if hop == 1 and array < 2 and array not in started:
            own[array].wait()
            started.add(array)
        for direction in range(2):
            if hop > 1:
                ring_copy(array, piece, hop - 1, direction, True).wait_recv()
                ring_copy(array, piece, hop - 1, direction, False).wait_send()
            if hop < n_sp:
                ring_copy(array, piece, hop, direction, False).start()

    first = [
        (array, piece, hop)
        for hop in range(1, n_sp)
        for array in range(2)
        for piece in range(splits)
    ]
    second = [(2, piece, hop) for hop in range(1, n_sp) for piece in range(splits)]
    queue = [first + second, 0]

    def advance(count):
        steps, at = queue
        for step in steps[at : at + count]:
            ring_step(*step)
        queue[1] = min(at + count, len(steps))

    unit = max(1, len(first) // 28)

    lat_own.wait()
    for hop in range(1, n_sp + 1):
        for direction in range(2):
            if hop > 1:
                lat_arrival(hop - 1, direction).wait_recv()
                lat_copy(hop - 1, direction).wait_send()
            if hop < n_sp:
                lat_copy(hop, direction).start()
            if hop > 2:
                share_copy(hop - 2, direction, core).wait_send()
            if hop > 1:
                share_copy(hop - 1, direction, core).start()
        if hop < n_sp and queue[1] < 7 * unit:
            advance(1)
        if preparing:
            preparing.pop(0)()
    while preparing:
        preparing.pop(0)()
    for direction in range(2):
        share_copy(n_sp - 1, direction, core).wait_send()
        for hop in range(1, n_sp):
            share_copy(hop, direction, 1 - core).wait_recv()

    total_rows = n_sp * n_rows
    lat_wide = lat_all.shape[3]
    chunk_blocks = max(1, min(n_sp, 1536 // n_rows))
    chunks = n_sp // chunk_blocks
    chunk = chunk_blocks * n_rows
    half_blocks = max(1, chunk_blocks // 2)

    def project(step):
        rows = half_blocks * n_rows
        blocks = pl.ds(step * half_blocks, half_blocks)
        lat = lat_all[blocks, :, :, pl.ds(0, rank)].reshape(rows, rank)
        rotary[pl.ds(step * rows, rows)] = lat_all[blocks, :, :, pl.ds(rank, LANES)].reshape(
            rows, LANES
        )
        keys[pl.ds(step * rows, rows)] = dot(lat, wk_ref[...]).astype(jnp.bfloat16)
        values[pl.ds(step * rows, rows)] = dot(lat, wv_ref[...]).astype(jnp.bfloat16)

    if chunks == 1:
        for step in range(n_sp // half_blocks):
            project(step)
            advance(unit)
    else:
        pl.loop(0, n_sp // half_blocks)(project)
        advance(2 * unit)

    score_scale = (NOPE + ROPE) ** (-0.5)
    lane = lax.broadcasted_iota(jnp.int32, (n_rows, LANES), 1)

    def attend(head, at, state):
        maxima, totals, running = state
        rows = pl.ds(at * chunk, chunk)
        pair = slice(head // 2 * LANES, (head // 2 + 1) * LANES)
        whole_keys = jnp.concatenate([keys[rows, pair], rotary[rows]], axis=1)
        scores = dot_nt(q_all[head], whole_keys) * score_scale
        top = jnp.max(scores, axis=1, keepdims=True)
        if maxima is not None:
            top = jnp.maximum(maxima, top)
        probs = jnp.exp(scores - top)
        sums = jnp.sum(probs, axis=1, keepdims=True)
        update = dot(probs.astype(jnp.bfloat16), values[rows, pair])
        if maxima is not None:
            factor = jnp.exp(maxima - top)
            sums = totals * factor + sums
            update = running * factor + update
        return (top, sums, update)

    for head in range(head_count):
        state = attend(head, 0, (None, None, None))
        if chunks > 1:
            state = lax.fori_loop(1, chunks, functools.partial(attend_loop, attend, head), state)
        result = state[2] / state[1]
        pair = slice(head // 2 * LANES, (head // 2 + 1) * LANES)
        if head % 2 == 0:
            heads[:, pair] = result.astype(jnp.bfloat16)
        else:
            heads[:, pair] = jnp.where(
                lane < VDIM, heads[:, pair].astype(jnp.float32), result
            ).astype(jnp.bfloat16)
        advance(unit)

    def tp_copy(stage, slot_source, slot_target, to, slot_semaphore):
        return pltpu.make_async_remote_copy(
            src_ref=slot_source,
            dst_ref=slot_target,
            send_sem=tp_send.at[stage, slot_semaphore],
            recv_sem=tp_recv.at[stage, slot_semaphore],
            device_id={"tp": to},
            device_id_type=MESH,
        )

    def exchange(stage, source_of, target_of):
        copies = []
        for k in range(1, n_tp):
            to = (tp + k) % n_tp
            copies.append(tp_copy(stage, source_of(to), target_of(k), to, k))
        return copies

    copies = exchange(0, lambda to: part_send.at[to], lambda k: part_recv.at[k])
    for k in range(1, n_tp + 1):
        to = (tp + k) % n_tp
        part_send[to] = dot(
            heads[...], wo_ref[:, pl.ds(pl.multiple_of(to * n_cols, LANES), n_cols)]
        ).astype(jnp.bfloat16)
        if k < n_tp:
            copies[k - 1].start()
    advance(4 * unit)
    mixed = DEEP_ALPHA * resid_ref[...].astype(jnp.float32) + part_send[tp].astype(jnp.float32)
    for k in range(1, n_tp):
        copies[k - 1].wait_recv()
        mixed = mixed + part_recv[k].astype(jnp.float32)
    pending = list(copies)

    width_total = n_cols * n_tp

    def normed(rows_in, gain_ref, stage, send, recv, between):
        sums = jnp.sum(rows_in, axis=1, keepdims=True)
        squares = jnp.sum(rows_in * rows_in, axis=1, keepdims=True)
        mine = jnp.transpose(jnp.where(lane < 4, sums, squares))[:8]
        send[...] = mine
        copies = exchange(stage, lambda to: send, lambda k: recv.at[k])
        for copy in copies:
            copy.start()
        between()
        for k in range(1, n_tp):
            copies[k - 1].wait_recv()
            mine = mine + recv[k]
        pending.extend(copies)
        whole = jnp.transpose(mine) / width_total
        row_mean = whole[:, :1]
        variance = whole[:, 4:5] - row_mean * row_mean
        return (
            (rows_in - row_mean) * lax.rsqrt(variance + NORM_EPSILON) * gain_ref[...]
        ).astype(jnp.bfloat16)

    hidden_in = normed(
        mixed, gain_mix_ref, 1, stat_send, stat_recv, lambda: advance(2 * unit)
    )
    rows_all[tp] = hidden_in
    copies = exchange(2, lambda to: rows_all.at[tp], lambda k: rows_all.at[tp])
    for copy in copies:
        copy.start()
    pending.extend(copies)
    advance(4 * unit)
    for k in range(1, n_tp):
        sender = (tp + n_tp - k) % n_tp
        tp_copy(2, rows_all.at[sender], rows_all.at[sender], sender, k).wait_recv()

    advance(len(first) - queue[1])
    advance(splits)

    def last_hop(array):
        for piece in range(splits):
            for direction in range(2):
                ring_copy(array, piece, n_sp - 1, direction, True).wait_recv()
                ring_copy(array, piece, n_sp - 1, direction, False).wait_send()

    last_hop(0)
    group = n_sp // n_tp
    depth = group * wg_ref.shape[0]
    hidden_width = wg_ref.shape[1]

    def wide(weight):
        total = None
        for t in range(n_tp):
            term = dot(
                rows_all[t],
                weight[t * group : (t + 1) * group].reshape(depth, hidden_width),
            )
            total = term if total is None else total + term
            advance(1)
        return total

    gate_sum = wide(gate_all)
    last_hop(1)
    up_sum = wide(up_all)
    hidden = (gate_sum / (1.0 + jnp.exp(-gate_sum)) * up_sum).astype(jnp.bfloat16)
    advance(1)

    half_rows = piece_rows * splits
    if half_rows % LANES == 0:
        hid[...] = hidden

        def down_copy(k, slot, to, columns):
            ref = part2_send.at[to, :, columns]
            return pltpu.make_async_remote_copy(
                src_ref=ref,
                dst_ref=part2_recv.at[k, :, columns],
                send_sem=down_send.at[k, slot],
                recv_sem=down_recv.at[k, slot],
                device_id={"tp": to},
                device_id_type=MESH,
            )

        def slot_columns(slot):
            return pl.ds(pl.multiple_of(slot * half_rows, LANES), half_rows)

        def make_columns(hop):
            for direction in range(2):
                block = origin(hop, direction)
                owner = block // group
                slot = (block % group) * 2 + direction
                rows = pl.ds(direction * half_rows, half_rows)
                part2_send[owner, :, slot_columns(slot)] = dot_nt(
                    hid[...], down_all[block, rows]
                ).astype(jnp.bfloat16)

                @pl.when(owner != tp)
                def send_away():
                    down_copy((owner + n_tp - tp) % n_tp, slot, owner, slot_columns(slot)).start()

        made = 0
        while queue[1] < len(queue[0]):
            array, piece, hop = queue[0][queue[1]]
            advance(1)
            if piece == splits - 1:
                made_to = hop
                while made < made_to:
                    make_columns(made)
                    made += 1
        while made < n_sp - 1:
            make_columns(made)
            made += 1
        last_hop(2)
        make_columns(n_sp - 1)
        mixer = part2_send[tp].astype(jnp.float32)
        for k in range(1, n_tp):
            for slot in range(2 * group):
                down_copy(k, slot, (tp + k) % n_tp, slot_columns(slot)).wait_recv()
            mixer = mixer + part2_recv[k].astype(jnp.float32)
    else:
        advance(len(queue[0]))
        last_hop(2)
        copies = exchange(3, lambda to: part2_send.at[to], lambda k: part2_recv.at[k])
        for k in range(1, n_tp + 1):
            to = (tp + k) % n_tp
            part2_send[to] = dot_nt(
                hidden, down_all[pl.ds(to * group, group)].reshape(depth, hidden_width)
            ).astype(jnp.bfloat16)
            if k < n_tp:
                copies[k - 1].start()
        mixer = part2_send[tp].astype(jnp.float32)
        for k in range(1, n_tp):
            copies[k - 1].wait_recv()
            mixer = mixer + part2_recv[k].astype(jnp.float32)
        pending.extend(copies)
    final = DEEP_ALPHA * rows_all[tp].astype(jnp.float32) + HALF_STEP * mixer
    out_ref[...] = normed(final, gain_out_ref, 4, stat2_send, stat2_recv, lambda: None)
    for copy in pending:
        copy.wait_send()
    if half_rows % LANES == 0:
        for k in range(1, n_tp):
            for slot in range(2 * group):
                down_copy(k, slot, (tp + k) % n_tp, slot_columns(slot)).wait_send()


def attend_loop(attend, head, at, state):
    return attend(head, at, state)


def local(
    queries,
    latents,
    rope_key,
    w_key,
    w_value,
    w_out,
    resid,
    gain_mix,
    w_gate,
    w_up,
    w_down,
    gain_out,
):
    n_sp = lax.axis_size("sp")
    n_tp = lax.axis_size("tp")
    rows = queries.shape[0]
    head_count = w_key.shape[1] // NOPE
    rank = latents.shape[1]
    cols = resid.shape[1]
    hidden_width = w_gate.shape[1]
    weight_rows = w_gate.shape[0]
    lat_wide = rank + LANES
    splits = 2 if weight_rows % 64 == 0 else 1
    bf16 = jnp.bfloat16
    total_rows = n_sp * rows
    vmem = pl.BlockSpec(memory_space=pltpu.VMEM)
    anywhere = pl.BlockSpec(memory_space=pl.ANY)
    dma = pltpu.SemaphoreType.DMA
    return pl.pallas_call(
        functools.partial(layer_kernel, n_sp, n_tp, splits),
        out_shape=jax.ShapeDtypeStruct((rows, cols), bf16),
        in_specs=[vmem, anywhere] + [vmem] * 7 + [anywhere] * 2 + [vmem],
        out_specs=vmem,
        scratch_shapes=[
            pltpu.VMEM((n_sp, 4, rows // 4, lat_wide), bf16),
            pltpu.VMEM((total_rows, head_count * NOPE), bf16),
            pltpu.VMEM((total_rows, LANES), bf16),
            pltpu.VMEM((total_rows, head_count * VDIM), bf16),
            pltpu.VMEM((n_sp, weight_rows, hidden_width), bf16),
            pltpu.VMEM((n_sp, weight_rows, hidden_width), bf16),
            pltpu.VMEM((n_sp, weight_rows, hidden_width), bf16),
            pltpu.VMEM((head_count, rows, 2 * LANES), bf16),
            pltpu.VMEM((rows, head_count * VDIM), bf16),
            pltpu.VMEM((n_tp, rows, cols), bf16),
            pltpu.VMEM((n_tp, rows, cols), bf16),
            pltpu.VMEM((8, rows), jnp.float32),
            pltpu.VMEM((n_tp, 8, rows), jnp.float32),
            pltpu.VMEM((n_tp, rows, cols), bf16),
            pltpu.VMEM((n_tp, rows, cols), bf16),
            pltpu.VMEM((n_tp, rows, cols), bf16),
            pltpu.VMEM((8, rows), jnp.float32),
            pltpu.VMEM((n_tp, 8, rows), jnp.float32),
            pltpu.VMEM((rows, hidden_width), bf16),
            dma((4,)),
            dma((2,)),
            dma((2, n_sp - 1)),
            dma((2,)),
            dma((2, n_sp - 1)),
            dma((3, splits, 2)),
            dma((3, splits, 2, n_sp - 1)),
            dma((5, n_tp)),
            dma((5, n_tp)),
            dma((n_tp, 2 * (n_sp // n_tp))),
            dma((n_tp, 2 * (n_sp // n_tp))),
        ],
        compiler_params=pltpu.CompilerParams(
            collective_id=0, has_side_effects=True, vmem_limit_bytes=66000000
        ),
    )(
        queries,
        latents.reshape(4, rows // 4, rank),
        rope_key,
        w_key,
        w_value,
        w_out,
        resid,
        gain_mix.reshape(1, -1),
        gain_out.reshape(1, -1),
        w_gate,
        w_up,
        w_down,
    )


def solution(mesh):
    placed = (
        P("sp", "tp"),
        P("sp", None),
        P("sp", None),
        P(None, "tp"),
        P(None, "tp"),
        P("tp", None),
        P("sp", "tp"),
        P("tp"),
        P("sp", "tp"),
        P("sp", "tp"),
        P("tp", "sp"),
        P("tp"),
    )
    return jax.shard_map(
        local, mesh=mesh, in_specs=placed, out_specs=P("sp", "tp"), check_vma=False
    )
```
